32 devices in a mesh: sp: 16 (over z, y, x), tp: 2 (over core).
Axes of the slice: x: 2, y: 2, z: 4, core: 2. Of those that a mesh axis runs over, the one named last changes fastest.
Arguments:
- gate_pre: bfloat16 [4096, 2048], P('sp', 'tp'), may hold values from -6 to 6
- conv_in: bfloat16 [4096, 2048], P('sp', 'tp'), may hold values from -6 to 6
- conv_taps: bfloat16 [4, 2048], P(None, 'tp'), may hold values from -3 to 3
- recur_map: bfloat16 [8, 256, 256], P('tp'), may hold values from -0.375 to 0.375
- input_map: bfloat16 [8, 256, 256], P('tp'), may hold values from -0.375 to 0.375
- rate_logit: float32 [2048], P('tp'), may hold values from 4.5 to 15
- decay_shift: float32 [4096, 8], P('sp', 'tp'), may hold values from -1.5 to 0
- out_weight: bfloat16 [2048, 2048], replicated, may hold values from -0.25 to 0.25
- residual: bfloat16 [4096, 2048], P(('sp', 'tp')), may hold values from -6 to 6
- gain_mix: float32 [2048], replicated, may hold values from 0.1 to 1.9
- routes: int32 [4096, 4], P(('sp', 'tp')), may hold values from 0 to 31, all different within a row; in each aligned block of 128 rows (0 to 127, 128 to 255, ...) at most 32 rows name the same one
- route_weight: float32 [4096, 4], P(('sp', 'tp')), may hold values from 0.2 to 1
- shared_gate: bfloat16 [2048, 512], replicated, may hold values from -0.125 to 0.125
- shared_up: bfloat16 [2048, 512], replicated, may hold values from -0.125 to 0.125
- shared_down: bfloat16 [512, 2048], replicated, may hold values from -0.375 to 0.375
- expert_gate: bfloat16 [32, 2048, 512], P(('sp', 'tp')), may hold values from -0.125 to 0.125
- expert_up: bfloat16 [32, 2048, 512], P(('sp', 'tp')), may hold values from -0.125 to 0.125
- expert_down: bfloat16 [32, 512, 2048], P(('sp', 'tp')), may hold values from -0.375 to 0.375
- gain_out: float32 [2048], replicated, may hold values from 0.1 to 1.9
Outputs:
- layer_out: bfloat16 [4096, 2048], P(('sp', 'tp'))
The draws below stay inside these ranges and needn't reach their ends.
Inputs may be any that keep to these rules, and one draw needn't show every extreme that they name: `routes`: each row names 4 different experts. In the rows of one device (aligned blocks of 128 rows) no expert is named more than 32 times, and in some blocks one expert is named exactly 32 times.
All inputs are finite; a program needn't handle non-finite values.
Results may differ from the reference program's by a relative error of at most 0.014.
Values may be sent and summed in bfloat16 or wider, within the bound.
A program may use at most 128 MiB of HBM per device.

```python
import math
import jax
import jax.numpy as jnp
import numpy as np
from jax import lax

D = 2048
HEADS = 8
BW = 256
DR = 2048
CONV = 4
FE = 512
FS = 512
TOPK = 4
TOKENS_PER_SHARD = 256
TOKENS = 4096
ROWS = 128
EXPERTS = 32
CAP = 32


def draw_rate_logit(key, part):
    flag_key, slow_key, fast_key = jax.random.split(jax.random.fold_in(key, 11), 3)
    fast_share = 0.5
    is_fast = jax.random.uniform(flag_key, (HEADS,), jnp.float32) < fast_share
    slow_rate = jnp.exp(jax.random.uniform(slow_key, (HEADS, BW), jnp.float32, math.log(0.3), math.log(1.2))) / TOKENS
    fast_rate = jnp.exp(jax.random.uniform(fast_key, (HEADS, BW), jnp.float32, math.log(0.02), math.log(0.067)))
    chosen_rate = jnp.where(is_fast[:, None], fast_rate, slow_rate)
    return (-jnp.log(jnp.expm1(chosen_rate / 8.0))).reshape(HEADS * BW).astype(jnp.float32)


def draw_decay_shift(key, part):
    base_key, place_key, size_key = jax.random.split(jax.random.fold_in(key, 23), 3)
    block_count = TOKENS // TOKENS_PER_SHARD
    lowest_value, highest = (0.1, 1.0)
    base = jnp.exp(jax.random.uniform(base_key, (block_count, HEADS), jnp.float32, math.log(lowest_value), math.log(highest))) / TOKENS
    equilibrium_memory = -jnp.repeat(base, TOKENS_PER_SHARD, axis=0)
    location_sequence = jax.random.randint(place_key, (2, HEADS), 0, TOKENS)
    objective_scores = jnp.log(jax.random.uniform(size_key, (2, HEADS), jnp.float32, 0.5, 0.8))
    ordinal_locator = jnp.arange(TOKENS)[:, None]
    arrival_clusters = jnp.where(ordinal_locator == location_sequence[0][None, :], objective_scores[0][None, :], 0.0) + jnp.where(ordinal_locator == location_sequence[1][None, :], objective_scores[1][None, :], 0.0)
    return (equilibrium_memory + arrival_clusters).astype(jnp.float32)


def block_scale(key, extent, cuts, least, top_value):
    def one(position, shards_of):
        steps = jax.random.uniform(jax.random.fold_in(jax.random.fold_in(key, 6), position), (shards_of,), jnp.float32, least / len(cuts), top_value / len(cuts))
        return jnp.repeat(jnp.exp(steps), extent[position] // shards_of).reshape((-1,) + (1,) * (len(extent) - position - 1))

    factor_of = one(*cuts[0])
    for cut in cuts[1:]:
        factor_of = factor_of * one(*cut)
    return factor_of


def assign_block(key, own, number, rows, number_of, top, most, slope):
    ranking = jax.random.permutation(key, number_of)
    packed, common = shares(number_of, rows * top, most, slope, True), shares(number_of, rows * top, most, slope, False)
    places = jnp.arange(number_of)

    def named(tallies, offset_by):
        used = int((tallies > 0).sum())
        fixed = max(1, used // 4)
        passed = fixed + (places - fixed + offset_by * (used - fixed)) % max(1, number_of - fixed)
        return jnp.zeros((number_of,), jnp.int32).at[ranking[jnp.where(places < fixed, places, passed)]].set(jnp.asarray(tallies, jnp.int32))

    tallies = jnp.where(number % 4 == 0, named(packed, number // 4), named(common, number - number // 4 - 1))
    mixed = jax.random.permutation(jax.random.fold_in(own, 3), number_of)
    giver, sink = mixed[0:number_of // 2 * 2:2], mixed[1:number_of // 2 * 2:2]
    slack = jnp.minimum(tallies[giver] - 1, most - tallies[sink]) // 2
    slack = jnp.where((giver == ranking[0]) | (sink == ranking[0]) | (tallies[sink] == 0), 0, jnp.maximum(slack, 0))
    passed = jax.random.randint(jax.random.fold_in(own, 4), (number_of // 2,), 0, 1 << 20) % (slack + 1)
    tallies = tallies.at[giver].add(-passed).at[sink].add(passed)
    labels = jnp.searchsorted(jnp.cumsum(tallies), jnp.arange(rows * top), side="right").astype(jnp.int32)
    listing = labels.reshape(top, rows).T
    listing = listing[jax.random.permutation(jax.random.fold_in(own, 1), rows)]
    offset_by = jax.random.randint(jax.random.fold_in(own, 2), (rows, 1), 0, top)
    return jnp.take_along_axis(listing, (jnp.arange(top)[None, :] + offset_by) % top, axis=1)


def shares(amount, total, bound, slope, full):
    loads = [(1 << 20) // math.isqrt(grade ** slope) + 1 for grade in range(1, amount + 1)]
    largest = bound if full else min(bound, max(-(-total // amount), total * loads[0] // sum(loads)))
    least = 1 if total - largest >= amount - 1 else 0
    given, spare = [largest] + [least] * (amount - 1), total - largest - least * (amount - 1)
    while spare > 0:
        free = [i for i in range(1, amount) if given[i] < largest] or [i for i in range(1, amount) if given[i] < bound]
        mass, left = sum([loads[i] for i in free]), spare
        for i in free:
            addition = min(bound - given[i], max(1, left * loads[i] // mass), spare)
            given[i] = given[i] + addition
            spare = spare - addition
    return np.array(given)


def centred(stream_key, shape, width, reach, cuts=(), kind=jnp.bfloat16):
    gain = block_scale(stream_key, shape, cuts, -0.22, 0.18) if cuts else 1.0
    drawn = jax.random.normal(stream_key, shape, jnp.float32) * width * gain
    return jnp.minimum(jnp.maximum(drawn, -reach), reach).astype(kind)


def setup_inputs(seed: int = 0) -> dict:
    streams_of = jax.random.split(jax.random.key(seed), 20)
    gate_pre = centred(streams_of[0], (TOKENS, DR), 1.0, 6.0, ((0, 16), (1, 2)))
    conv_in = centred(streams_of[1], (TOKENS, DR), 1.0, 6.0, ((0, 16), (1, 2)))
    conv_taps = centred(streams_of[2], (CONV, DR), CONV ** -0.5, 3.0, ((1, 2),))
    recur_map = centred(streams_of[3], (HEADS, BW, BW), BW ** -0.5, 0.375, ((0, 2),))
    input_map = centred(streams_of[4], (HEADS, BW, BW), BW ** -0.5, 0.375, ((0, 2),))
    rate_logit = draw_rate_logit(jax.random.fold_in(streams_of[19], 71), 0)
    decay_shift = draw_decay_shift(jax.random.fold_in(streams_of[19], 71), 0)
    out_weight = centred(streams_of[7], (DR, D), (DR // 4) ** -0.5, 0.25)
    residual = centred(streams_of[8], (TOKENS, D), 1.0, 6.0, ((0, 32),))
    gain_mix = jnp.clip(1.0 + 0.18 * jax.random.normal(streams_of[9], (D,), jnp.float32), 0.1, 1.9)
    routes_keys = jax.random.split(jax.random.fold_in(streams_of[10], 1), TOKENS // ROWS)
    routes_turns = jax.random.permutation(jax.random.fold_in(streams_of[10], 3), TOKENS // ROWS)
    routes = jax.vmap(lambda own, number: assign_block(jax.random.fold_in(streams_of[10], 2), own, number, ROWS, EXPERTS, TOPK, CAP, 1))(routes_keys, routes_turns).reshape((TOKENS, TOPK))
    route_weight = jnp.clip(0.2 + 0.8 * jax.random.uniform(streams_of[11], (TOKENS, TOPK), jnp.float32) ** block_scale(streams_of[11], (TOKENS, TOPK), ((0, 32),), -0.2, 0.2), 0.2, 1.0)
    shared_gate = centred(streams_of[12], (D, FS), D ** -0.5, 0.125)
    shared_up = centred(streams_of[13], (D, FS), D ** -0.5, 0.125)
    shared_down = centred(streams_of[14], (FS, D), (FS // 2) ** -0.5, 0.375)
    expert_gate = centred(streams_of[15], (EXPERTS, D, FE), D ** -0.5, 0.125, ((0, 32),))
    expert_up = centred(streams_of[16], (EXPERTS, D, FE), D ** -0.5, 0.125, ((0, 32),))
    expert_down = centred(streams_of[17], (EXPERTS, FE, D), (FE // 2) ** -0.5, 0.375, ((0, 32),))
    gain_out = jnp.clip(1.0 + 0.18 * jax.random.normal(streams_of[18], (D,), jnp.float32), 0.1, 1.9)
    return dict(gate_pre=gate_pre, conv_in=conv_in, conv_taps=conv_taps, recur_map=recur_map, input_map=input_map, rate_logit=rate_logit, decay_shift=decay_shift, out_weight=out_weight, residual=residual, gain_mix=gain_mix, routes=routes, route_weight=route_weight, shared_gate=shared_gate, shared_up=shared_up, shared_down=shared_down, expert_gate=expert_gate, expert_up=expert_up, expert_down=expert_down, gain_out=gain_out)


ALPHA = 8.0 ** 0.25
RATE_C = 8.0
NORM_EPS = 1e-05

def layer_norm(values, gains):
    center = values - lax.optimization_barrier(jnp.mean(values, axis=-1, keepdims=True))
    spread = lax.optimization_barrier(jnp.mean(center * center, axis=-1, keepdims=True))
    return center * lax.rsqrt(spread + NORM_EPS) * gains

def combine(former, latter):
    return (former[0] * latter[0], latter[0] * former[1] + latter[1])

def reference(gate_pre, conv_in, conv_taps, recur_map, input_map, rate_logit, decay_shift, out_weight, residual, gain_mix, routes, route_weight, shared_gate, shared_up, shared_down, expert_gate, expert_up, expert_down, gain_out):
    length = conv_in.shape[0]
    padded = jnp.concatenate([jnp.zeros((CONV - 1, DR), conv_in.dtype), conv_in], axis=0).astype(jnp.float32)
    filter_tap_weight = conv_taps.astype(jnp.float32)
    summed = jnp.zeros((length, DR), jnp.float32)
    for offset in range(CONV):
        summed = summed + filter_tap_weight[offset] * padded[offset:offset + length]
    conv_out = summed.astype(jnp.bfloat16)
    grouped = conv_out.astype(jnp.float32).reshape(length, HEADS, BW)
    recur_gate = jax.nn.sigmoid(jnp.einsum('thc,hcd->thd', grouped, recur_map.astype(jnp.float32)))
    input_gate = jax.nn.sigmoid(jnp.einsum('thc,hcd->thd', grouped, input_map.astype(jnp.float32)))
    log_decay = -RATE_C * jax.nn.softplus(-rate_logit).reshape(HEADS, BW) * recur_gate + decay_shift[:, :, None]
    update = jnp.sqrt(-jnp.expm1(2.0 * log_decay)) * input_gate * grouped
    states = lax.associative_scan(combine, (jnp.exp(log_decay), update), axis=0)[1]
    mixed_rows = (states.reshape(length, DR) * jax.nn.gelu(gate_pre.astype(jnp.float32), approximate=True)).astype(jnp.bfloat16)
    projected = jnp.dot(mixed_rows, out_weight, preferred_element_type=jnp.float32)
    normed = layer_norm(ALPHA * residual.astype(jnp.float32) + projected, gain_mix).astype(jnp.bfloat16)
    fanout = routes.shape[1]
    flat_ids = routes.reshape(-1).astype(jnp.int32)
    ordering = jnp.argsort(flat_ids, stable=True).astype(jnp.int32)
    sorted_ids = flat_ids[ordering]
    counts = jax.ops.segment_sum(jnp.ones_like(flat_ids), flat_ids, num_segments=EXPERTS).astype(jnp.int32)
    starts = (jnp.cumsum(counts) - counts).astype(jnp.int32)
    within = (jnp.arange(flat_ids.shape[0], dtype=jnp.int32) - starts[sorted_ids]).astype(jnp.int32)
    most_rows = length // ROWS * CAP
    sources = jnp.full((EXPERTS, most_rows), length, jnp.int32).at[sorted_ids, within].set(ordering // fanout)
    weights = jnp.zeros((EXPERTS, most_rows), jnp.float32).at[sorted_ids, within].set(route_weight.reshape(-1)[ordering].astype(jnp.float32))
    padded_rows = jnp.concatenate([normed, jnp.zeros((1, D), jnp.bfloat16)], axis=0)

    def specialist_pass(routed, member):
        chosen_ids, chosen_weights, gate_weight, up_weight, down_weight = member
        chosen = padded_rows[chosen_ids]
        hidden = (jax.nn.silu(jnp.dot(chosen, gate_weight, preferred_element_type=jnp.float32)) * jnp.dot(chosen, up_weight, preferred_element_type=jnp.float32)).astype(jnp.bfloat16)
        result = jnp.dot(hidden, down_weight, preferred_element_type=jnp.float32).astype(jnp.bfloat16)
        return (routed.at[chosen_ids].add(chosen_weights[:, None] * result.astype(jnp.float32)), None)
    routed = lax.scan(specialist_pass, jnp.zeros((length + 1, D), jnp.float32), (sources, weights, expert_gate, expert_up, expert_down))[0]
    shared_hidden = (jax.nn.silu(jnp.dot(normed, shared_gate, preferred_element_type=jnp.float32)) * jnp.dot(normed, shared_up, preferred_element_type=jnp.float32)).astype(jnp.bfloat16)
    moe_sum = jnp.dot(shared_hidden, shared_down, preferred_element_type=jnp.float32) + routed[:length]
    return layer_norm(ALPHA * normed.astype(jnp.float32) + moe_sum, gain_out).astype(jnp.bfloat16)
```

```python
import functools

import jax
import jax.numpy as jnp
from jax import lax
from jax.experimental import pallas as pl
from jax.experimental.pallas import tpu as pltpu
from jax.sharding import PartitionSpec as P

ALPHA = 8.0**0.25
RATE_C = 8.0
NORM_EPS = 1e-05
MESH = pl.DeviceIdType.MESH


def from_behind(block, axis, distance):
    devices = range(lax.axis_size(axis))
    route = [(i - distance, i) for i in devices if i - distance in devices]
    return lax.ppermute(block, axis, route)


def expm1_of_negative(y):
    series = jnp.ones_like(y)
    for order in range(8, 1, -1):
        series = 1.0 + series * y * (1.0 / order)
    return jnp.where(y > -0.35, y * series, jnp.exp(y) - 1.0)


def recurrence_kernel(
    before_ref, conv_ref, taps_ref, recur_ref, input_ref, coef_ref, shift_ref, run_ref, state_ref, tail_ref
):
    tokens, width = conv_ref.shape
    reach = taps_ref.shape[0] - 1
    x = conv_ref[...].astype(jnp.float32)
    before = before_ref[...]
    taps = taps_ref[...].astype(jnp.float32)
    top_row = lax.broadcasted_iota(jnp.int32, (8, width), 0)
    summed = jnp.zeros((tokens, width), jnp.float32)
    for offset in range(reach + 1):
        back = reach - offset
        if back:
            moved = pltpu.roll(x, back, 0)
            first = jnp.where(top_row < back, pltpu.roll(before, back, 0), moved[:8])
            moved = jnp.concatenate([first, moved[8:]], axis=0)
        else:
            moved = x
        summed = summed + taps[offset : offset + 1] * moved
    conv_out = summed.astype(jnp.bfloat16)
    recur_gate = jax.nn.sigmoid(jnp.dot(conv_out, recur_ref[0], preferred_element_type=jnp.float32))
    input_gate = jax.nn.sigmoid(jnp.dot(conv_out, input_ref[0], preferred_element_type=jnp.float32))
    shifts = shift_ref[...]
    column = lax.broadcasted_iota(jnp.int32, shifts.shape, 1)
    shift = jnp.sum(jnp.where(column == pl.program_id(0), shifts, 0.0), axis=1, keepdims=True)
    log_decay = coef_ref[...] * recur_gate + shift
    update = jnp.sqrt(-expm1_of_negative(2.0 * log_decay)) * input_gate * conv_out.astype(jnp.float32)
    run, state = jnp.exp(log_decay), update
    row = lax.broadcasted_iota(jnp.int32, (tokens, width), 0)
    step = 1
    while step < tokens:
        if step < 8:
            inside = row >= step
            run_before = jnp.where(inside, pltpu.roll(run, step, 0), 1.0)
            state_before = jnp.where(inside, pltpu.roll(state, step, 0), 0.0)
        else:
            run_before = jnp.concatenate([jnp.ones((step, width), jnp.float32), run[:-step]], axis=0)
            state_before = jnp.concatenate([jnp.zeros((step, width), jnp.float32), state[:-step]], axis=0)
        state = state + run * state_before
        run = run * run_before
        step *= 2
    run_ref[...] = run
    state_ref[...] = state
    tail_ref[...] = jnp.where(top_row == 7, run[tokens - 8 :], pltpu.roll(state[tokens - 8 :], 7, 0))


def recurrence(before, conv_in, conv_taps, recur_map, input_map, coef, decay_shift):
    tokens, channels = conv_in.shape
    heads, width = recur_map.shape[:2]
    return pl.pallas_call(
        recurrence_kernel,
        grid=(heads,),
        in_specs=[
            pl.BlockSpec((8, width), lambda h: (0, h)),
            pl.BlockSpec((tokens, width), lambda h: (0, h)),
            pl.BlockSpec((conv_taps.shape[0], width), lambda h: (0, h)),
            pl.BlockSpec((1, width, width), lambda h: (h, 0, 0)),
            pl.BlockSpec((1, width, width), lambda h: (h, 0, 0)),
            pl.BlockSpec((1, width), lambda h: (0, h)),
            pl.BlockSpec((tokens, heads), lambda h: (0, 0)),
        ],
        out_specs=[
            pl.BlockSpec((tokens, width), lambda h: (0, h)),
            pl.BlockSpec((tokens, width), lambda h: (0, h)),
            pl.BlockSpec((8, width), lambda h: (0, h)),
        ],
        out_shape=[
            jax.ShapeDtypeStruct((tokens, channels), jnp.float32),
            jax.ShapeDtypeStruct((tokens, channels), jnp.float32),
            jax.ShapeDtypeStruct((8, channels), jnp.float32),
        ],
    )(before, conv_in, conv_taps, recur_map, input_map, coef, decay_shift)


def entering_kernel(count, tail_ref, out_ref, land, send_sem, recv_sem):
    me, core = lax.axis_index("sp"), lax.axis_index("tp")
    barrier = pltpu.get_barrier_semaphore()
    for d in range(1, count):
        pl.semaphore_signal(barrier, inc=1, device_id=(lax.rem(me + d, count), core), device_id_type=MESH)
    pl.semaphore_wait(barrier, count - 1)
    copies = []
    for d in range(1, count):
        copy = pltpu.make_async_remote_copy(
            src_ref=tail_ref,
            dst_ref=land.at[d],
            send_sem=send_sem.at[d],
            recv_sem=recv_sem.at[d],
            device_id=(lax.rem(me + d, count), core),
            device_id_type=MESH,
        )
        copy.start()
        copies.append(copy)
    for copy in copies:
        copy.wait()
    carry = jnp.zeros((1, tail_ref.shape[1]), jnp.float32)
    for d in range(count - 1, 0, -1):
        longer = land[d, 7:8] * carry + land[d, 6:7]
        carry = jnp.where(jnp.full(carry.shape, d, jnp.int32) <= me, longer, carry)
    out_ref[...] = carry


def entering(tail):
    count = lax.axis_size("sp")
    return pl.pallas_call(
        functools.partial(entering_kernel, count),
        out_shape=jax.ShapeDtypeStruct((1, tail.shape[1]), jnp.float32),
        in_specs=[pl.BlockSpec(memory_space=pltpu.VMEM)],
        out_specs=pl.BlockSpec(memory_space=pltpu.VMEM),
        scratch_shapes=[
            pltpu.VMEM((count, *tail.shape), jnp.float32),
            pltpu.SemaphoreType.DMA((count,)),
            pltpu.SemaphoreType.DMA((count,)),
        ],
        compiler_params=pltpu.CompilerParams(collective_id=0, has_side_effects=True),
    )(tail)


def layer_norm(values, gains):
    center = values - jnp.mean(values, axis=-1, keepdims=True)
    spread = jnp.mean(center * center, axis=-1, keepdims=True)
    return center * lax.rsqrt(spread + NORM_EPS) * gains


def on_device(
    gate_pre,
    conv_in,
    conv_taps,
    recur_map,
    input_map,
    rate_logit,
    decay_shift,
    out_weight,
    residual,
    gain_mix,
    routes,
    route_weight,
    shared_gate,
    shared_up,
    shared_down,
    expert_gate,
    expert_up,
    expert_down,
    gain_out,
):
    tokens, channels = conv_in.shape
    reach = conv_taps.shape[0] - 1
    before = from_behind(conv_in[tokens - reach :], "sp", 1).astype(jnp.float32)
    before = jnp.concatenate([jnp.zeros((8 - reach, channels), jnp.float32), before], axis=0)
    coef = (-RATE_C * jax.nn.softplus(-rate_logit)).reshape(1, channels)
    running, local_state, tail = recurrence(
        before, conv_in, conv_taps, recur_map, input_map, coef, decay_shift
    )
    states = local_state + running * entering(tail)
    mixed_rows = (states * jax.nn.gelu(gate_pre.astype(jnp.float32), approximate=True)).astype(jnp.bfloat16)
    row_count = tokens // lax.axis_size("tp")
    regrouped = lax.all_to_all(mixed_rows, "tp", split_axis=0, concat_axis=1, tiled=True)
    projected = jnp.dot(regrouped, out_weight, preferred_element_type=jnp.float32)
    normed = layer_norm(ALPHA * residual.astype(jnp.float32) + projected, gain_mix).astype(
        jnp.bfloat16
    )
    model_width = normed.shape[1]
    fanout = routes.shape[1]
    sp_count, tp_count = (lax.axis_size("sp"), lax.axis_size("tp"))
    experts = sp_count * tp_count
    capacity = max(2, 2 * row_count * fanout // experts)
    entries = row_count * fanout
    flat_ids = routes.reshape(entries)
    onehot = (flat_ids[:, None] == lax.iota(jnp.int32, experts)[None, :]).astype(jnp.bfloat16)
    before_mask = (
        lax.iota(jnp.int32, entries)[:, None] > lax.iota(jnp.int32, entries)[None, :]
    ).astype(jnp.bfloat16)
    earlier = jnp.dot(before_mask, onehot, preferred_element_type=jnp.float32)
    slot_rank = jnp.sum(earlier * onehot.astype(jnp.float32), axis=1).astype(jnp.int32)
    slot_index = flat_ids * capacity + slot_rank
    source_row = (
        jnp.full((experts * capacity,), row_count, jnp.int32)
        .at[slot_index]
        .set(lax.iota(jnp.int32, entries) // fanout)
    )
    padded_rows = jnp.concatenate([normed, jnp.zeros((1, model_width), jnp.bfloat16)], axis=0)
    outgoing = padded_rows[source_row].reshape(experts, capacity, model_width)
    shared_hidden = (
        jax.nn.silu(jnp.dot(normed, shared_gate, preferred_element_type=jnp.float32))
        * jnp.dot(normed, shared_up, preferred_element_type=jnp.float32)
    ).astype(jnp.bfloat16)
    shared_out = jnp.dot(shared_hidden, shared_down, preferred_element_type=jnp.float32)
    received = lax.all_to_all(outgoing, ("sp", "tp"), split_axis=0, concat_axis=0, tiled=True)
    senders = received.shape[0]
    slot_count = received.shape[1]
    chosen = received.reshape(senders * slot_count, model_width)
    hidden = (
        jax.nn.silu(jnp.dot(chosen, expert_gate[0], preferred_element_type=jnp.float32))
        * jnp.dot(chosen, expert_up[0], preferred_element_type=jnp.float32)
    ).astype(jnp.bfloat16)
    handed_result = lax.all_to_all(
        jnp.dot(hidden, expert_down[0], preferred_element_type=jnp.float32)
        .astype(jnp.bfloat16)
        .reshape(senders, slot_count, model_width),
        ("sp", "tp"),
        split_axis=0,
        concat_axis=0,
        tiled=True,
    )
    gathered = handed_result.reshape(experts * capacity, model_width)[slot_index].reshape(
        row_count, fanout, model_width
    )
    moe_sum = shared_out + jnp.sum(route_weight[:, :, None] * gathered.astype(jnp.float32), axis=1)
    return layer_norm(ALPHA * normed.astype(jnp.float32) + moe_sum, gain_out).astype(jnp.bfloat16)


def solution(mesh):
    return jax.shard_map(
        on_device,
        mesh=mesh,
        in_specs=(
            P("sp", "tp"),
            P("sp", "tp"),
            P(None, "tp"),
            P("tp", None, None),
            P("tp", None, None),
            P("tp"),
            P("sp", "tp"),
            P(),
            P(("sp", "tp"), None),
            P(),
            P(("sp", "tp"), None),
            P(("sp", "tp"), None),
            P(),
            P(),
            P(),
            P(("sp", "tp"), None, None),
            P(("sp", "tp"), None, None),
            P(("sp", "tp"), None, None),
            P(),
        ),
        out_specs=P(("sp", "tp"), None),
        check_vma=False,
    )
```

```python
import functools

import jax
import jax.numpy as jnp
from jax import lax
from jax.experimental import pallas as pl
from jax.experimental.pallas import tpu as pltpu
from jax.sharding import PartitionSpec as P

ALPHA = 8.0**0.25
RATE_C = 8.0
NORM_EPS = 1e-05
MESH = pl.DeviceIdType.MESH


def from_behind(block, axis, distance):
    devices = range(lax.axis_size(axis))
    route = [(i - distance, i) for i in devices if i - distance in devices]
    return lax.ppermute(block, axis, route)


def expm1_of_negative(y):
    series = jnp.ones_like(y)
    for order in range(8, 1, -1):
        series = 1.0 + series * y * (1.0 / order)
    return jnp.where(y > -0.35, y * series, jnp.exp(y) - 1.0)


def recurrence_kernel(
    before_ref, conv_ref, taps_ref, recur_ref, input_ref, coef_ref, shift_ref, run_ref, state_ref, tail_ref
):
    tokens, width = conv_ref.shape
    reach = taps_ref.shape[0] - 1
    x = conv_ref[...].astype(jnp.float32)
    before = before_ref[...]
    taps = taps_ref[...].astype(jnp.float32)
    top_row = lax.broadcasted_iota(jnp.int32, (8, width), 0)
    summed = jnp.zeros((tokens, width), jnp.float32)
    for offset in range(reach + 1):
        back = reach - offset
        if back:
            moved = pltpu.roll(x, back, 0)
            first = jnp.where(top_row < back, pltpu.roll(before, back, 0), moved[:8])
            moved = jnp.concatenate([first, moved[8:]], axis=0)
        else:
            moved = x
        summed = summed + taps[offset : offset + 1] * moved
    conv_out = summed.astype(jnp.bfloat16)
    recur_gate = jax.nn.sigmoid(jnp.dot(conv_out, recur_ref[0], preferred_element_type=jnp.float32))
    input_gate = jax.nn.sigmoid(jnp.dot(conv_out, input_ref[0], preferred_element_type=jnp.float32))
    shifts = shift_ref[...]
    column = lax.broadcasted_iota(jnp.int32, shifts.shape, 1)
    shift = jnp.sum(jnp.where(column == pl.program_id(0), shifts, 0.0), axis=1, keepdims=True)
    log_decay = coef_ref[...] * recur_gate + shift
    update = jnp.sqrt(-expm1_of_negative(2.0 * log_decay)) * input_gate * conv_out.astype(jnp.float32)
    run, state = jnp.exp(log_decay), update
    row = lax.broadcasted_iota(jnp.int32, (tokens, width), 0)
    step = 1
    while step < tokens:
        if step < 8:
            inside = row >= step
            run_before = jnp.where(inside, pltpu.roll(run, step, 0), 1.0)
            state_before = jnp.where(inside, pltpu.roll(state, step, 0), 0.0)
        else:
            run_before = jnp.concatenate([jnp.ones((step, width), jnp.float32), run[:-step]], axis=0)
            state_before = jnp.concatenate([jnp.zeros((step, width), jnp.float32), state[:-step]], axis=0)
        state = state + run * state_before
        run = run * run_before
        step *= 2
    run_ref[...] = run
    state_ref[...] = state
    tail_ref[...] = jnp.where(top_row == 7, run[tokens - 8 :], pltpu.roll(state[tokens - 8 :], 7, 0))


def recurrence(before, conv_in, conv_taps, recur_map, input_map, coef, decay_shift):
    tokens, channels = conv_in.shape
    heads, width = recur_map.shape[:2]
    return pl.pallas_call(
        recurrence_kernel,
        grid=(heads,),
        in_specs=[
            pl.BlockSpec((8, width), lambda h: (0, h)),
            pl.BlockSpec((tokens, width), lambda h: (0, h)),
            pl.BlockSpec((conv_taps.shape[0], width), lambda h: (0, h)),
            pl.BlockSpec((1, width, width), lambda h: (h, 0, 0)),
            pl.BlockSpec((1, width, width), lambda h: (h, 0, 0)),
            pl.BlockSpec((1, width), lambda h: (0, h)),
            pl.BlockSpec((tokens, heads), lambda h: (0, 0)),
        ],
        out_specs=[
            pl.BlockSpec((tokens, width), lambda h: (0, h)),
            pl.BlockSpec((tokens, width), lambda h: (0, h)),
            pl.BlockSpec((8, width), lambda h: (0, h)),
        ],
        out_shape=[
            jax.ShapeDtypeStruct((tokens, channels), jnp.float32),
            jax.ShapeDtypeStruct((tokens, channels), jnp.float32),
            jax.ShapeDtypeStruct((8, channels), jnp.float32),
        ],
    )(before, conv_in, conv_taps, recur_map, input_map, coef, decay_shift)


def entering_kernel(count, tail_ref, out_ref, land, send_sem, recv_sem):
    me, core = lax.axis_index("sp"), lax.axis_index("tp")
    barrier = pltpu.get_barrier_semaphore()
    for d in range(1, count):
        pl.semaphore_signal(barrier, inc=1, device_id=(lax.rem(me + d, count), core), device_id_type=MESH)
    pl.semaphore_wait(barrier, count - 1)
    copies = []
    for d in range(1, count):
        copy = pltpu.make_async_remote_copy(
            src_ref=tail_ref,
            dst_ref=land.at[d],
            send_sem=send_sem.at[d],
            recv_sem=recv_sem.at[d],
            device_id=(lax.rem(me + d, count), core),
            device_id_type=MESH,
        )
        copy.start()
        copies.append(copy)
    for copy in copies:
        copy.wait()
    carry = jnp.zeros((1, tail_ref.shape[1]), jnp.float32)
    for d in range(count - 1, 0, -1):
        longer = land[d, 7:8] * carry + land[d, 6:7]
        carry = jnp.where(jnp.full(carry.shape, d, jnp.int32) <= me, longer, carry)
    out_ref[...] = carry


def entering(tail):
    count = lax.axis_size("sp")
    return pl.pallas_call(
        functools.partial(entering_kernel, count),
        out_shape=jax.ShapeDtypeStruct((1, tail.shape[1]), jnp.float32),
        in_specs=[pl.BlockSpec(memory_space=pltpu.VMEM)],
        out_specs=pl.BlockSpec(memory_space=pltpu.VMEM),
        scratch_shapes=[
            pltpu.VMEM((count, *tail.shape), jnp.float32),
            pltpu.SemaphoreType.DMA((count,)),
            pltpu.SemaphoreType.DMA((count,)),
        ],
        compiler_params=pltpu.CompilerParams(collective_id=0, has_side_effects=True),
    )(tail)


def layer_norm(values, gains):
    center = values - jnp.mean(values, axis=-1, keepdims=True)
    spread = jnp.mean(center * center, axis=-1, keepdims=True)
    return center * lax.rsqrt(spread + NORM_EPS) * gains


def experts_kernel(
    outer,
    inner,
    cores,
    capacity,
    rows_ref,
    meta_ref,
    shared_gate_ref,
    shared_up_ref,
    shared_down_ref,
    gate_ref,
    up_ref,
    down_ref,
    out_ref,
    rows,
    meta,
    packed,
    arrived,
    result,
    back,
    part,
    part_land,
    row_sems,
    meta_sems,
    go_sems,
    back_sems,
    part_sems,
):
    sp, core = lax.axis_index("sp"), lax.axis_index("tp")
    layer, place = sp // inner, lax.rem(sp, inner) * cores + core
    plane = inner * cores
    slots = plane * capacity
    fanout = meta_ref.shape[0] // 2

    def along(d):
        return (lax.rem(layer + d + outer, outer) * inner + lax.rem(sp, inner), core)

    def across(d):
        other = lax.rem(place + d + plane, plane)
        return (layer * inner + other // cores, lax.rem(other, cores))

    def remote(src, dst, sems, index, device):
        return pltpu.make_async_remote_copy(
            src_ref=src,
            dst_ref=dst,
            send_sem=sems.at[(0, *index)],
            recv_sem=sems.at[(1, *index)],
            device_id=device,
            device_id_type=MESH,
        )

    def row_copy(d):
        return remote(rows_ref, rows.at[d], row_sems, (d,), along(d))

    def meta_copy(d):
        return remote(meta_ref, meta.at[d], meta_sems, (d,), along(d))

    def piece(ref, b, d):
        return ref.at[b, pl.ds(d * capacity, capacity)]

    def go_copy(b, d):
        return remote(piece(packed, b, d), piece(arrived, b, d), go_sems, (b, d), across(d))

    def back_copy(b, d):
        return remote(piece(result, b, d), piece(back, b, d), back_sems, (b, d), across(-d))

    def part_copy(b):
        return remote(part.at[b], part_land.at[b], part_sems, (b,), along(-b))

    barrier = pltpu.get_barrier_semaphore()
    for d in range(1, outer):
        pl.semaphore_signal(barrier, inc=1, device_id=along(d), device_id_type=MESH)
    for d in range(1, plane):
        pl.semaphore_signal(barrier, inc=1, device_id=across(d), device_id_type=MESH)
    pl.semaphore_wait(barrier, outer + plane - 2)
    for d in range(1, outer):
        meta_copy(d).start()
        row_copy(d).start()
    rows[0] = rows_ref[...]
    meta[0] = meta_ref[...]

    def wanted(b):
        width = meta_ref.shape[1]
        slot = lax.broadcasted_iota(jnp.int32, (slots, width), 0) + place * capacity
        slot = jnp.where(slot >= slots, slot - slots, slot) + layer * slots
        return slot.astype(jnp.float32)

    def weighed(b, ones):
        slot = wanted(b)
        total = jnp.zeros(slot.shape, jnp.float32)
        for k in range(fanout):
            value = 1.0 if ones else meta[b, fanout + k : fanout + k + 1]
            total = total + jnp.where(slot == meta[b, k : k + 1], value, 0.0)
        return total

    def pack(b):
        chosen = jnp.dot(
            weighed(b, True).astype(jnp.bfloat16), rows[b], preferred_element_type=jnp.float32
        ).astype(jnp.bfloat16)
        packed[b] = chosen
        arrived[b, :capacity] = chosen[:capacity]
        for d in range(1, plane):
            go_copy(b, d).start()

    def gated(x, gate, up, down):
        hidden = (
            jax.nn.silu(jnp.dot(x, gate, preferred_element_type=jnp.float32))
            * jnp.dot(x, up, preferred_element_type=jnp.float32)
        ).astype(jnp.bfloat16)
        return jnp.dot(hidden, down, preferred_element_type=jnp.float32)

    pack(0)
    out_ref[...] = gated(rows_ref[...], shared_gate_ref[...], shared_up_ref[...], shared_down_ref[...])

    def turn(step, carry):
        @pl.when(step < outer)
        def _():
            meta_copy(step).wait()
            row_copy(step).wait()
            pack(step)

        @pl.when(step <= outer)
        def _():
            b = step - 1
            for d in range(1, plane):
                go_copy(b, d).wait()
            done = gated(arrived[b], gate_ref[0], up_ref[0], down_ref[0]).astype(jnp.bfloat16)
            result[b] = done
            back[b, :capacity] = done[:capacity]
            for d in range(1, plane):
                back_copy(b, d).start()

        @pl.when(step >= 2)
        def _():
            b = step - 2
            for d in range(1, plane):
                back_copy(b, d).wait()
            weight = weighed(b, False).T
            high = weight.astype(jnp.bfloat16)
            low = (weight - high.astype(jnp.float32)).astype(jnp.bfloat16)
            summed = jnp.dot(high, back[b], preferred_element_type=jnp.float32) + jnp.dot(
                low, back[b], preferred_element_type=jnp.float32
            )

            @pl.when(b == 0)
            def _():
                out_ref[...] += summed

            @pl.when(b > 0)
            def _():
                part[b] = summed.astype(jnp.bfloat16)
                part_copy(b).start()

        return carry

    lax.fori_loop(1, outer + 2, turn, 0)
    for b in range(1, outer):
        part_copy(b).wait()
        out_ref[...] += part_land[b].astype(jnp.float32)


def experts_sum(normed, meta, capacity, weights):
    sp_count, cores = lax.axis_size("sp"), lax.axis_size("tp")
    outer = 4 if sp_count % 4 == 0 else 1
    inner = sp_count // outer
    plane = inner * cores
    rows, width = normed.shape
    bf16 = lambda *shape: pltpu.VMEM((*shape, width), jnp.bfloat16)
    sems = lambda *shape: pltpu.SemaphoreType.DMA((2, *shape))
    slots = plane * capacity
    return pl.pallas_call(
        functools.partial(experts_kernel, outer, inner, cores, capacity),
        out_shape=jax.ShapeDtypeStruct((rows, width), jnp.float32),
        in_specs=[pl.BlockSpec(memory_space=pltpu.VMEM)] * 8,
        out_specs=pl.BlockSpec(memory_space=pltpu.VMEM),
        scratch_shapes=[
            bf16(outer, rows),
            pltpu.VMEM((outer, *meta.shape), jnp.float32),
            bf16(outer, slots),
            bf16(outer, slots),
            bf16(outer, slots),
            bf16(outer, slots),
            bf16(outer, rows),
            bf16(outer, rows),
            sems(outer),
            sems(outer),
            sems(outer, plane),
            sems(outer, plane),
            sems(outer),
        ],
        compiler_params=pltpu.CompilerParams(collective_id=1, has_side_effects=True),
    )(normed, meta, *weights)


def on_device(
    gate_pre,
    conv_in,
    conv_taps,
    recur_map,
    input_map,
    rate_logit,
    decay_shift,
    out_weight,
    residual,
    gain_mix,
    routes,
    route_weight,
    shared_gate,
    shared_up,
    shared_down,
    expert_gate,
    expert_up,
    expert_down,
    gain_out,
):
    tokens, channels = conv_in.shape
    reach = conv_taps.shape[0] - 1
    before = from_behind(conv_in[tokens - reach :], "sp", 1).astype(jnp.float32)
    before = jnp.concatenate([jnp.zeros((8 - reach, channels), jnp.float32), before], axis=0)
    coef = (-RATE_C * jax.nn.softplus(-rate_logit)).reshape(1, channels)
    running, local_state, tail = recurrence(
        before, conv_in, conv_taps, recur_map, input_map, coef, decay_shift
    )
    states = local_state + running * entering(tail)
    mixed_rows = (states * jax.nn.gelu(gate_pre.astype(jnp.float32), approximate=True)).astype(jnp.bfloat16)
    row_count = tokens // lax.axis_size("tp")
    regrouped = lax.all_to_all(mixed_rows, "tp", split_axis=0, concat_axis=1, tiled=True)
    projected = jnp.dot(regrouped, out_weight, preferred_element_type=jnp.float32)
    normed = layer_norm(ALPHA * residual.astype(jnp.float32) + projected, gain_mix).astype(
        jnp.bfloat16
    )
    fanout = routes.shape[1]
    sp_count, tp_count = (lax.axis_size("sp"), lax.axis_size("tp"))
    experts = sp_count * tp_count
    capacity = max(2, 2 * row_count * fanout // experts)
    entries = row_count * fanout
    flat_ids = routes.reshape(entries)
    onehot = (flat_ids[:, None] == lax.iota(jnp.int32, experts)[None, :]).astype(jnp.bfloat16)
    before_mask = (
        lax.iota(jnp.int32, entries)[:, None] > lax.iota(jnp.int32, entries)[None, :]
    ).astype(jnp.bfloat16)
    earlier = jnp.dot(before_mask, onehot, preferred_element_type=jnp.float32)
    slot_rank = jnp.sum(earlier * onehot.astype(jnp.float32), axis=1).astype(jnp.int32)
    slot_index = flat_ids * capacity + slot_rank
    meta = jnp.concatenate(
        [slot_index.reshape(row_count, fanout).T.astype(jnp.float32), route_weight.T], axis=0
    )
    moe_sum = experts_sum(
        normed,
        meta,
        capacity,
        (shared_gate, shared_up, shared_down, expert_gate, expert_up, expert_down),
    )
    return layer_norm(ALPHA * normed.astype(jnp.float32) + moe_sum, gain_out).astype(jnp.bfloat16)


def solution(mesh):
    return jax.shard_map(
        on_device,
        mesh=mesh,
        in_specs=(
            P("sp", "tp"),
            P("sp", "tp"),
            P(None, "tp"),
            P("tp", None, None),
            P("tp", None, None),
            P("tp"),
            P("sp", "tp"),
            P(),
            P(("sp", "tp"), None),
            P(),
            P(("sp", "tp"), None),
            P(("sp", "tp"), None),
            P(),
            P(),
            P(),
            P(("sp", "tp"), None, None),
            P(("sp", "tp"), None, None),
            P(("sp", "tp"), None, None),
            P(),
        ),
        out_specs=P(("sp", "tp"), None),
        check_vma=False,
    )
```
